32 devices in a mesh: sp: 8 (over z, y), dp: 4 (over x, core).
Axes of the slice: x: 2, y: 2, z: 4, core: 2. Of those that a mesh axis runs over, the one named last changes fastest.
Arguments:
- queries: bfloat16 [4, 1024, 1024], P('dp', 'sp'), may hold values from -6 to 6
- keys: bfloat16 [4, 1024, 256], P('dp', 'sp'), may hold values from -6 to 6
- values: bfloat16 [4, 1024, 256], P('dp', 'sp'), may hold values from -6 to 6
- q_gain: float32 [64], replicated, may hold values from 0.55 to 8
- k_gain: float32 [64], replicated, may hold values from 0.55 to 8
- residual: bfloat16 [4, 1024, 2048], P('dp', 'sp'), may hold values from -6 to 6
- out_weight: bfloat16 [1024, 2048], replicated, may hold values from -0.1875 to 0.1875
- mix_gain: float32 [2048], replicated, may hold values from 0.1 to 1.9
- ffn_gain: float32 [2048], replicated, may hold values from 0.1 to 1.9
- post_gain: float32 [2048], replicated, may hold values from 0.1 to 1.9
- expert_ids: int32 [4, 1024, 2], P('dp', 'sp'), may hold values from 0 to 31, all different within a row; in each aligned block of 128 rows (0 to 127, 128 to 255, ..., all dimensions but the last counted through in order) at most 16 rows name the same one
- expert_gate: float32 [4, 1024, 2], P('dp', 'sp'), may hold values from 0.05 to 1
- w_gate: bfloat16 [32, 2048, 512], P(('sp', 'dp')), may hold values from -0.125 to 0.125
- w_up: bfloat16 [32, 2048, 512], P(('sp', 'dp')), may hold values from -0.125 to 0.125
- w_down: bfloat16 [32, 512, 2048], P(('sp', 'dp')), may hold values from -0.25 to 0.25
Outputs:
- result: bfloat16 [4, 1024, 2048], P('dp', 'sp')
The draws below stay inside these ranges and needn't reach their ends.
Inputs may be any that keep to these rules, and one draw needn't show every extreme that they name: `expert_ids`: each token names 2 different experts; among the 128 tokens of one device no expert is named more than 16 times, and that bound is reached.
All inputs are finite; a program needn't handle non-finite values.
Results may differ from the reference program's by a relative error of at most 0.0085.
The reference program's roundings to bfloat16 on the way count: a program that leaves them out, or rounds other values in their place, can miss the bound.
Values may be sent and summed in bfloat16 or wider, within the bound.
A program may use at most 64 MiB of HBM per device.

```python
import math
import jax
import jax.numpy as jnp
import numpy as np
from jax import lax

D = 2048
HEAD = 64
H_Q = 16
H_KV = 4
DE = 512
TOP = 2
GRID = 64
TOK_DEV = 128
SEQS = 4
LEN = 1024
EXPERTS = 32
CAP = 16
N_SP = 8
N_DP = 4


def key_field(key):
    base = jax.random.normal(jax.random.fold_in(key, 23), (SEQS, LEN, H_KV * HEAD), jnp.float32)
    return jnp.clip(base, -6.0, 6.0)


def draw_keys(key, part):
    return key_field(key).astype(jnp.bfloat16)


def draw_queries(key, part):
    base = jax.random.normal(jax.random.fold_in(key, 11), (SEQS, LEN, H_Q * HEAD), jnp.float32)
    base = jnp.clip(base, -6.0, 6.0)
    return base.astype(jnp.bfloat16)


def draw_q_gain(key, part):
    inner = jax.random.fold_in(key, 41)
    return 1.0 + 0.18 * jnp.clip(jax.random.normal(inner, (HEAD,), jnp.float32), -2.5, 2.5)


def draw_k_gain(key, part):
    inner = jax.random.fold_in(key, 43)
    return 1.0 + 0.18 * jnp.clip(jax.random.normal(inner, (HEAD,), jnp.float32), -2.5, 2.5)


def level_of(own_key, dims, pieces, least, largest):
    level = 1.0
    for dim, blocks in pieces:
        draws = jax.random.uniform(jax.random.fold_in(jax.random.fold_in(own_key, 6), dim), (blocks,), jnp.float32, least / len(pieces), largest / len(pieces))
        level = level * jnp.repeat(jnp.exp(draws), dims[dim] // blocks).reshape((-1,) + (1,) * (len(dims) - 1 - dim))
    return level


def routed_block(own_key, own, number, rows, count, top, reach, lean):
    ranking = jax.random.permutation(own_key, count)
    crowded, ordinary = load_shares(count, rows * top, reach, lean, True), load_shares(count, rows * top, reach, lean, False)
    places = jnp.arange(count)

    def named(lengths, turn):
        used = int((lengths > 0).sum())
        fixed = max(1, used // 4)
        passed = fixed + (places - fixed + turn * (used - fixed)) % max(1, count - fixed)
        return jnp.zeros((count,), jnp.int32).at[ranking[jnp.where(places < fixed, places, passed)]].set(jnp.asarray(lengths, jnp.int32))

    lengths = jnp.where(number % 4 == 0, named(crowded, number // 4), named(ordinary, number - number // 4 - 1))
    mixed = jax.random.permutation(jax.random.fold_in(own, 3), count)
    giver, sink = mixed[0:count // 2 * 2:2], mixed[1:count // 2 * 2:2]
    slack = jnp.minimum(lengths[giver] - 1, reach - lengths[sink]) // 2
    slack = jnp.where((giver == ranking[0]) | (sink == ranking[0]) | (lengths[sink] == 0), 0, jnp.maximum(slack, 0))
    passed = jax.random.randint(jax.random.fold_in(own, 4), (count // 2,), 0, 1 << 20) % (slack + 1)
    lengths = lengths.at[giver].add(-passed).at[sink].add(passed)
    members = jnp.searchsorted(jnp.cumsum(lengths), jnp.arange(rows * top), side="right").astype(jnp.int32)
    listing = members.reshape(top, rows).T
    listing = listing[jax.random.permutation(jax.random.fold_in(own, 1), rows)]
    turn = jax.random.randint(jax.random.fold_in(own, 2), (rows, 1), 0, top)
    return jnp.take_along_axis(listing, (jnp.arange(top)[None, :] + turn) % top, axis=1)


def load_shares(number_of, total, most, slope, full):
    portions = [(1 << 20) // math.isqrt(grade ** slope) + 1 for grade in range(1, number_of + 1)]
    largest = most if full else min(most, max(-(-total // number_of), total * portions[0] // sum(portions)))
    least = 1 if total - largest >= number_of - 1 else 0
    holding, spare = [largest] + [least] * (number_of - 1), total - largest - least * (number_of - 1)
    while spare > 0:
        movable = [i for i in range(1, number_of) if holding[i] < largest] or [i for i in range(1, number_of) if holding[i] < most]
        mass, left = sum([portions[i] for i in movable]), spare
        for i in movable:
            addition = min(most - holding[i], max(1, left * portions[i] // mass), spare)
            holding[i] = holding[i] + addition
            spare = spare - addition
    return np.array(holding)


def scatter_about(stream_key, dims, width, bound, cuts=(), kind=jnp.bfloat16):
    drawn = width * jax.random.normal(stream_key, dims, jnp.float32)
    if cuts:
        drawn = drawn * level_of(stream_key, dims, cuts, -0.22, 0.18)
    return jnp.clip(drawn, -bound, bound).astype(kind)


def setup_inputs(seed: int = 0) -> dict:
    splits = jax.random.split(jax.random.key(seed), 16)
    queries = draw_queries(jax.random.fold_in(splits[15], 71), 0)
    keys = draw_keys(jax.random.fold_in(splits[15], 71), 0)
    values = scatter_about(splits[2], (SEQS, LEN, H_KV * HEAD), 1.0, 6.0, ((0, 4), (1, 8)))
    q_gain = draw_q_gain(jax.random.fold_in(splits[15], 71), 0)
    k_gain = draw_k_gain(jax.random.fold_in(splits[15], 71), 0)
    residual = scatter_about(splits[5], (SEQS, LEN, D), 1.0, 6.0, ((0, 4), (1, 8)))
    out_weight = scatter_about(splits[6], (H_Q * HEAD, D), (H_Q * HEAD) ** -0.5, 0.1875)
    mix_gain = jnp.clip(1.0 + 0.18 * jax.random.normal(splits[7], (D,), jnp.float32), 0.1, 1.9)
    ffn_gain = jnp.clip(1.0 + 0.18 * jax.random.normal(splits[8], (D,), jnp.float32), 0.1, 1.9)
    post_gain = jnp.clip(1.0 + 0.18 * jax.random.normal(splits[9], (D,), jnp.float32), 0.1, 1.9)
    expert_ids_keys = jax.random.split(jax.random.fold_in(splits[10], 1), SEQS * LEN // TOK_DEV)
    expert_ids_turns = jax.random.permutation(jax.random.fold_in(splits[10], 3), SEQS * LEN // TOK_DEV)
    expert_ids = jax.vmap(lambda own, number: routed_block(jax.random.fold_in(splits[10], 2), own, number, TOK_DEV, EXPERTS, TOP, CAP, 2))(expert_ids_keys, expert_ids_turns).reshape((SEQS, LEN, TOP))
    expert_gate = jnp.clip(jnp.exp(math.log(1.0) - 2.9957323 * jax.random.uniform(splits[11], (SEQS, LEN, TOP), jnp.float32) ** level_of(splits[11], (SEQS, LEN, TOP), ((0, 4), (1, 8)), -0.2, 0.2)), 0.05, 1.0)
    w_gate = scatter_about(splits[12], (EXPERTS, D, DE), D ** -0.5, 0.125, ((0, 32),))
    w_up = scatter_about(splits[13], (EXPERTS, D, DE), D ** -0.5, 0.125, ((0, 32),))
    w_down = scatter_about(splits[14], (EXPERTS, DE, D), DE ** -0.5, 0.25, ((0, 32),))
    return {"queries": queries, "keys": keys, "values": values, "q_gain": q_gain, "k_gain": k_gain, "residual": residual, "out_weight": out_weight, "mix_gain": mix_gain, "ffn_gain": ffn_gain, "post_gain": post_gain, "expert_ids": expert_ids, "expert_gate": expert_gate, "w_gate": w_gate, "w_up": w_up, "w_down": w_down}


eps_norm = 1e-06
theta_base = 10000.0
block_rows = 512

def rms_scale(values):
    return values * lax.rsqrt(lax.optimization_barrier(jnp.mean(values * values, axis=-1, keepdims=True)) + eps_norm)

def rotate(field, gain):
    seq_len, head_count, head_size = field.shape
    values = rms_scale(field.astype(jnp.float32)) * gain
    positions = jnp.arange(seq_len, dtype=jnp.int32)
    row_index = (positions // GRID).astype(jnp.float32)
    col_index = (positions % GRID).astype(jnp.float32)
    pair_quarter = head_size // 4
    frequency = theta_base ** (-(4.0 * jnp.arange(pair_quarter, dtype=jnp.float32)) / head_size)
    angles = jnp.concatenate([row_index[:, None] * frequency, col_index[:, None] * frequency], axis=1)
    cosine_table = jnp.cos(angles)[:, None, :]
    sine_table = jnp.sin(angles)[:, None, :]
    paired = values.reshape(seq_len, head_count, head_size // 2, 2)
    even_part = paired[..., 0]
    odd_part = paired[..., 1]
    turned = jnp.stack([even_part * cosine_table - odd_part * sine_table, even_part * sine_table + odd_part * cosine_table], axis=-1)
    return turned.reshape(seq_len, head_count, head_size).astype(jnp.bfloat16)

def attend(q_turned, k_turned, v_rows):
    seq_len, q_count, head_size = q_turned.shape
    kv_count = k_turned.shape[1]
    group_size = q_count // kv_count
    k_float = k_turned.astype(jnp.float32)
    v_float = v_rows.astype(jnp.float32)

    def one_block(start):
        q_block = lax.dynamic_slice_in_dim(q_turned, start, block_rows, 0)
        q_block = q_block.reshape(block_rows, kv_count, group_size, head_size).astype(jnp.float32)
        scores = jnp.einsum('qkgd,skd->kgqs', q_block, k_float) * head_size ** (-0.5)
        row_max = lax.optimization_barrier(jnp.max(scores, axis=-1, keepdims=True))
        exp_scores = jnp.exp(scores - row_max)
        weights = (exp_scores / lax.optimization_barrier(jnp.sum(exp_scores, axis=-1, keepdims=True))).astype(jnp.bfloat16)
        summed = jnp.einsum('kgqs,skd->qkgd', weights.astype(jnp.float32), v_float)
        return summed.astype(jnp.bfloat16).reshape(block_rows, q_count * head_size)
    starts = jnp.arange(seq_len // block_rows, dtype=jnp.int32) * block_rows
    return lax.map(one_block, starts).reshape(seq_len, q_count * head_size)

def reference(queries, keys, values, q_gain, k_gain, residual, out_weight, mix_gain, ffn_gain, post_gain, expert_ids, expert_gate, w_gate, w_up, w_down):
    seq_count, seq_len, q_width = queries.shape
    head_size = q_gain.shape[0]

    def per_sequence(items):
        q_seq, k_seq, v_seq = items
        q_turned = rotate(q_seq.reshape(seq_len, -1, head_size), q_gain)
        k_turned = rotate(k_seq.reshape(seq_len, -1, head_size), k_gain)
        return attend(q_turned, k_turned, v_seq.reshape(seq_len, -1, head_size))
    attended = lax.map(per_sequence, (queries, keys, values)).reshape(-1, q_width)
    projected = jnp.dot(attended, out_weight, preferred_element_type=jnp.float32)
    first_res = (residual.reshape(-1, D).astype(jnp.float32) + rms_scale(projected) * mix_gain).astype(jnp.bfloat16)
    normed = (rms_scale(first_res.astype(jnp.float32)) * ffn_gain).astype(jnp.bfloat16)
    flat_ids = expert_ids.reshape(-1).astype(jnp.int32)
    flat_gate = expert_gate.reshape(-1)
    slot_count = N_SP * N_DP * CAP

    def per_expert(running_sum, number):
        matches = flat_ids == number
        picked = jnp.nonzero(matches, size=slot_count, fill_value=0)[0].astype(jnp.int32)
        live_mask = (jnp.arange(slot_count, dtype=jnp.int32) < jnp.sum(matches.astype(jnp.int32))).astype(jnp.float32)
        token_rows = (picked // TOP).astype(jnp.int32)
        inputs = normed[token_rows]
        gate_value = jnp.dot(inputs, w_gate[number], preferred_element_type=jnp.float32)
        up_value = jnp.dot(inputs, w_up[number], preferred_element_type=jnp.float32)
        hidden = (jax.nn.silu(gate_value) * up_value).astype(jnp.bfloat16)
        expert_out = jnp.dot(hidden, w_down[number], preferred_element_type=jnp.float32).astype(jnp.bfloat16)
        weight = flat_gate[picked] * live_mask
        return (running_sum.at[token_rows].add(weight[:, None] * expert_out.astype(jnp.float32)), None)
    expert_sum, _ = lax.scan(per_expert, jnp.zeros((normed.shape[0], D), jnp.float32), jnp.arange(EXPERTS, dtype=jnp.int32))
    result = (first_res.astype(jnp.float32) + rms_scale(expert_sum) * post_gain).astype(jnp.bfloat16)
    return result.reshape(seq_count, seq_len, D)
```

```python
import functools

import jax
import jax.numpy as jnp
import numpy as np
from jax import lax
from jax.experimental import pallas as pl
from jax.experimental.pallas import tpu as pltpu
from jax.sharding import PartitionSpec as P

GRID = 64
LANES = 128
eps_norm = 1e-06
theta_base = 10000.0
MESH = pl.DeviceIdType.MESH
f32 = jnp.float32
bf16 = jnp.bfloat16


def tables(rows, head_size):
    half = head_size // 2
    lane = np.arange(LANES) % head_size
    pair = lane // 2
    quarter = head_size // 4
    by_row = pair < quarter
    frequency = theta_base ** (-(4.0 * (pair % quarter)) / head_size)
    sign = np.where(lane % 2 == 0, -1.0, 1.0)
    a_row = np.arange(rows)[:, None] * frequency
    a_col = np.arange(GRID)[:, None] * frequency
    out = (
        np.where(by_row, np.cos(a_row), 0.0),
        np.where(by_row, np.sin(a_row) * sign, 0.0),
        np.where(by_row, 0.0, np.cos(a_col)),
        np.where(by_row, 0.0, np.sin(a_col) * sign),
    )
    return [jnp.asarray(t, f32) for t in out]


def rms(x):
    return x * lax.rsqrt(jnp.mean(x * x, axis=-1, keepdims=True) + eps_norm)


def dot(a, b):
    return jnp.dot(a, b, preferred_element_type=f32)


def kernel(
    n_sp, n_dp, cap, pitch, groups,
    q_ref, k_ref, v_ref, qg_ref, kg_ref, cr_ref, sr_ref, cc_ref, sc_ref,
    res_ref, mix_ref, ffn_ref, post_ref, ids_ref, gate_ref,
    wo_hbm, wg_hbm, wu_hbm, wd_hbm,
    out_ref,
    kbuf, vbuf, att, first, outbox, arrived, returned, pack, comb_hi, comb_lo,
    wo, wg, wu, wd, w_sem,
    ks_send, ks_recv, vs_send, vs_recv, d_send, d_recv, r_send, r_recv,
):
    n_dev = n_sp * n_dp
    sp = lax.axis_index("sp")
    dp = lax.axis_index("dp")
    tok, q_width = q_ref.shape
    kv_width = k_ref.shape[1]
    head = qg_ref.shape[1]
    d_model = res_ref.shape[1]
    heads_q, heads_kv = q_width // head, kv_width // head
    group = heads_q // heads_kv

    weights = [
        pltpu.make_async_copy(src, dst, w_sem.at[n])
        for n, (src, dst) in enumerate(((wo_hbm, wo), (wg_hbm, wg), (wu_hbm, wu), (wd_hbm, wd)))
    ]
    for w in weights:
        w.start()

    def peer(i):
        return lax.rem(sp + i // n_dp, n_sp), lax.rem(dp + i % n_dp, n_dp)

    def source(i):
        return lax.rem(sp + n_sp - i // n_dp, n_sp), lax.rem(dp + n_dp - i % n_dp, n_dp)

    barrier = pltpu.get_barrier_semaphore()

    def greet(i, c):
        pl.semaphore_signal(barrier, inc=1, device_id=peer(i), device_id_type=MESH)
        return c

    lax.fori_loop(1, n_dev, greet, 0)

    lane = lax.broadcasted_iota(jnp.int32, (tok, LANES), 1)
    even = lane % 2 == 0
    low = lane % (2 * head) < head
    same = (
        lax.broadcasted_iota(jnp.int32, (LANES, LANES), 0) // head
        == lax.broadcasted_iota(jnp.int32, (LANES, LANES), 1) // head
    ).astype(bf16)
    per_dev = tok // GRID
    cos_t = jnp.concatenate(
        [cc_ref[...] + cr_ref[pl.ds(sp * per_dev + u, 1), :] for u in range(per_dev)], axis=0
    )
    sin_t = jnp.concatenate(
        [sc_ref[...] + sr_ref[pl.ds(sp * per_dev + u, 1), :] for u in range(per_dev)], axis=0
    )

    def turn(x, gain):
        x = x.astype(f32)
        square = x * x
        hi = square.astype(bf16)
        lo = (square - hi.astype(f32)).astype(bf16)
        mean = (dot(hi, same) + dot(lo, same)) * (1.0 / head)
        x = x * lax.rsqrt(mean + eps_norm) * gain
        swapped = jnp.where(even, pltpu.roll(x, LANES - 1, 1), pltpu.roll(x, 1, 1))
        return x * cos_t + swapped * sin_t

    k_gain = jnp.concatenate([kg_ref[...]] * (LANES // head), axis=1)
    q_gain = jnp.concatenate([qg_ref[...]] * (LANES // head), axis=1)
    for c in range(kv_width // LANES):
        cols = slice(c * LANES, (c + 1) * LANES)
        kbuf[0, :, cols] = turn(k_ref[:, cols], k_gain).astype(bf16)
    vbuf[0] = v_ref[...]

    pl.semaphore_wait(barrier, n_dev - 1)

    def kv_copies(i):
        to = (lax.rem(sp + i, n_sp), dp)
        return (
            pltpu.make_async_remote_copy(
                kbuf.at[0], kbuf.at[i], ks_send.at[i], ks_recv.at[i], device_id=to, device_id_type=MESH
            ),
            pltpu.make_async_remote_copy(
                v_ref, vbuf.at[i], vs_send.at[i], vs_recv.at[i], device_id=to, device_id_type=MESH
            ),
        )

    def kv_start(i, c):
        a, b = kv_copies(i)
        a.start()
        b.start()
        return c

    lax.fori_loop(1, n_sp, kv_start, 0)

    q_rows = [[] for _ in range(heads_kv)]
    per_chunk = LANES // head
    for c in range(q_width // LANES):
        x = turn(q_ref[:, c * LANES : (c + 1) * LANES], q_gain) * head ** (-0.5)
        for part in range(per_chunk):
            kv = (c * per_chunk + part) // group
            want = kv % per_chunk
            y = x if part == want else pltpu.roll(x, head, 1)
            keep = low if want == 0 else jnp.logical_not(low)
            q_rows[kv].append(jnp.where(keep, y, 0.0).astype(bf16))

    n_slot = n_dev * pitch
    e_iota = lax.broadcasted_iota(jnp.int32, (n_dev, tok), 0)
    hit0 = (e_iota == ids_ref[0:1, :]).astype(f32)
    hit1 = (e_iota == ids_ref[1:2, :]).astype(f32)
    hits = hit0 + hit1
    before = (
        lax.broadcasted_iota(jnp.int32, (tok, tok), 0) < lax.broadcasted_iota(jnp.int32, (tok, tok), 1)
    ).astype(bf16)
    rank = dot(hits.astype(bf16), before)
    mark = (hits * (rank + 1.0)).astype(bf16)
    spread = (
        lax.broadcasted_iota(jnp.int32, (n_slot, n_dev), 0) // pitch
        == lax.broadcasted_iota(jnp.int32, (n_slot, n_dev), 1)
    ).astype(bf16)
    place = (lax.broadcasted_iota(jnp.int32, (n_slot, tok), 0) % pitch + 1).astype(f32)
    chosen = dot(spread, mark) == place
    pack[...] = chosen.astype(f32).astype(bf16)
    g = gate_ref[...]
    g_hi = g.astype(bf16).astype(f32)
    g_lo = g - g_hi
    for dst, part in ((comb_hi, g_hi), (comb_lo, g_lo)):
        both = (hit0 * part[0:1, :] + hit1 * part[1:2, :]).astype(bf16)
        dst[...] = jnp.where(chosen, dot(spread, both), 0.0).astype(bf16)

    def kv_wait(i, c):
        a, b = kv_copies(i)
        a.wait()
        b.wait()
        return c

    lax.fori_loop(1, n_sp, kv_wait, 0)

    keys = n_sp * tok
    outs = {}
    for kv in range(heads_kv):
        cols = slice(kv // per_chunk * LANES, (kv // per_chunk + 1) * LANES)
        k_all = kbuf[:, :, cols].reshape(keys, LANES)
        v_all = vbuf[:, :, cols].reshape(keys, LANES)
        for part in range(group):
            s = lax.dot_general(
                q_rows[kv][part], k_all, (((1,), (1,)), ((), ())), preferred_element_type=f32
            )
            p = jnp.exp(s - jnp.max(s, axis=-1, keepdims=True))
            total = jnp.sum(p, axis=-1, keepdims=True)
            outs[kv * group + part] = dot(p.astype(bf16), v_all) / total
    for c in range(q_width // LANES):
        piece = None
        for part in range(per_chunk):
            h = c * per_chunk + part
            have = (h // group) % per_chunk
            y = outs[h] if part == have else pltpu.roll(outs[h], head, 1)
            piece = y if piece is None else jnp.where(low, piece, y)
        att[:, c * LANES : (c + 1) * LANES] = piece.astype(bf16)

    weights[0].wait()
    projected = dot(att[...], wo[...])
    mixed = (res_ref[...].astype(f32) + rms(projected) * mix_ref[...]).astype(bf16)
    first[...] = mixed
    normed = (rms(mixed.astype(f32)) * ffn_ref[...]).astype(bf16)
    outbox[...] = dot(pack[...], normed).astype(bf16).reshape(n_dev, pitch, d_model)

    per_group = n_dev // groups
    order = [g_ for g_ in (2, 1, 3, 0) if g_ < groups]

    def dispatch(i):
        to = peer(i)
        return pltpu.make_async_remote_copy(
            outbox.at[to[0] * n_dp + to[1]], arrived.at[i], d_send.at[i], d_recv.at[i],
            device_id=to, device_id_type=MESH,
        )

    def answer(i):
        return pltpu.make_async_remote_copy(
            arrived.at[i], returned.at[sp * n_dp + dp], r_send.at[i], r_recv.at[i],
            device_id=source(i), device_id_type=MESH,
        )

    def start_d(i, c):
        dispatch(i).start()
        return c

    def wait_d(i, c):
        dispatch(i).wait()
        return c

    def start_r(i, c):
        answer(i).start()
        return c

    def wait_r(i, c):
        answer(i).wait()
        return c

    for gi in order:
        lax.fori_loop(max(gi * per_group, 1), (gi + 1) * per_group, start_d, 0)
    me = sp * n_dp + dp
    arrived[0] = outbox[me]
    for w in weights[1:]:
        w.wait()
    for gi in order:
        lo_, hi_ = gi * per_group, (gi + 1) * per_group
        lax.fori_loop(max(lo_, 1), hi_, wait_d, 0)
        x = arrived[lo_:hi_].reshape(per_group * pitch, d_model)
        gate_value = dot(x, wg[...])
        up_value = dot(x, wu[...])
        hidden = (gate_value / (1.0 + jnp.exp(-gate_value)) * up_value).astype(bf16)
        y = dot(hidden, wd[...]).astype(bf16)
        arrived[lo_:hi_] = y.reshape(per_group, pitch, d_model)
        lax.fori_loop(max(lo_, 1), hi_, start_r, 0)
    returned[me] = arrived[0]
    for gi in order:
        lax.fori_loop(max(gi * per_group, 1), (gi + 1) * per_group, wait_r, 0)

    back = returned[...].reshape(n_slot, d_model)
    dims = (((0,), (0,)), ((), ()))
    expert_sum = lax.dot_general(comb_hi[...], back, dims, preferred_element_type=f32)
    expert_sum += lax.dot_general(comb_lo[...], back, dims, preferred_element_type=f32)
    out_ref[...] = (first[...].astype(f32) + rms(expert_sum) * post_ref[...]).astype(bf16)


def shards(
    queries, keys, values, q_gain, k_gain, residual, out_weight, mix_gain, ffn_gain, post_gain,
    expert_ids, expert_gate, w_gate, w_up, w_down,
):
    n_sp = lax.axis_size("sp")
    n_dp = lax.axis_size("dp")
    n_dev = n_sp * n_dp
    tok = queries.shape[1]
    d_model = residual.shape[2]
    d_exp = w_gate.shape[2]
    head = q_gain.shape[0]
    kv_width = keys.shape[2]
    q_width = queries.shape[2]
    cap = 2 * tok * expert_ids.shape[2] // n_dev
    pitch = -(-cap // 16) * 16
    n_slot = n_dev * pitch
    vmem = pl.BlockSpec(memory_space=pltpu.VMEM)
    hbm = pl.BlockSpec(memory_space=pl.ANY)
    dma = pltpu.SemaphoreType.DMA
    result = pl.pallas_call(
        functools.partial(kernel, n_sp, n_dp, cap, pitch, 4),
        out_shape=jax.ShapeDtypeStruct((tok, d_model), bf16),
        in_specs=[vmem] * 15 + [hbm] * 4,
        out_specs=vmem,
        scratch_shapes=[
            pltpu.VMEM((n_sp, tok, kv_width), bf16),
            pltpu.VMEM((n_sp, tok, kv_width), bf16),
            pltpu.VMEM((tok, q_width), bf16),
            pltpu.VMEM((tok, d_model), bf16),
            pltpu.VMEM((n_dev, pitch, d_model), bf16),
            pltpu.VMEM((n_dev, pitch, d_model), bf16),
            pltpu.VMEM((n_dev, pitch, d_model), bf16),
            pltpu.VMEM((n_slot, tok), bf16),
            pltpu.VMEM((n_slot, tok), bf16),
            pltpu.VMEM((n_slot, tok), bf16),
            pltpu.VMEM((q_width, d_model), bf16),
            pltpu.VMEM((d_model, d_exp), bf16),
            pltpu.VMEM((d_model, d_exp), bf16),
            pltpu.VMEM((d_exp, d_model), bf16),
            dma((4,)),
            dma((n_sp,)), dma((n_sp,)), dma((n_sp,)), dma((n_sp,)),
            dma((n_dev,)), dma((n_dev,)), dma((n_dev,)), dma((n_dev,)),
        ],
        compiler_params=pltpu.CompilerParams(
            collective_id=0, has_side_effects=True, vmem_limit_bytes=63000000
        ),
    )(
        queries[0], keys[0], values[0], q_gain[None], k_gain[None],
        *tables(n_sp * tok // GRID, head),
        residual[0], mix_gain[None], ffn_gain[None], post_gain[None],
        expert_ids[0].T, expert_gate[0].T,
        out_weight, w_gate[0], w_up[0], w_down[0],
    )
    return result[None]


def solution(mesh):
    tokens = P("dp", "sp", None)
    experts = P(("sp", "dp"), None, None)
    return jax.shard_map(
        shards,
        mesh=mesh,
        in_specs=(tokens, tokens, tokens, P(), P(), tokens, P(), P(), P(), P(), tokens, tokens,
                  experts, experts, experts),
        out_specs=tokens,
        check_vma=False,
    )
```

```python
import functools

import jax
import jax.numpy as jnp
import numpy as np
from jax import lax
from jax.experimental import pallas as pl
from jax.experimental.pallas import tpu as pltpu
from jax.sharding import PartitionSpec as P

GRID = 64
LANES = 128
eps_norm = 1e-06
theta_base = 10000.0
MESH = pl.DeviceIdType.MESH
f32 = jnp.float32
bf16 = jnp.bfloat16


def tables(rows, head_size):
    half = head_size // 2
    lane = np.arange(LANES) % head_size
    pair = lane // 2
    quarter = head_size // 4
    by_row = pair < quarter
    frequency = theta_base ** (-(4.0 * (pair % quarter)) / head_size)
    sign = np.where(lane % 2 == 0, -1.0, 1.0)
    a_row = np.arange(rows)[:, None] * frequency
    a_col = np.arange(GRID)[:, None] * frequency
    out = (
        np.where(by_row, np.cos(a_row), 0.0),
        np.where(by_row, np.sin(a_row) * sign, 0.0),
        np.where(by_row, 0.0, np.cos(a_col)),
        np.where(by_row, 0.0, np.sin(a_col) * sign),
    )
    return [jnp.asarray(t, f32) for t in out]


def rms(x):
    return x * lax.rsqrt(jnp.mean(x * x, axis=-1, keepdims=True) + eps_norm)


def dot(a, b):
    return jnp.dot(a, b, preferred_element_type=f32)


def kernel(
    n_sp, n_dp, pitch,
    q_ref, k_ref, v_ref, qg_ref, kg_ref, cr_ref, sr_ref, cc_ref, sc_ref,
    res_ref, mix_ref, ffn_ref, post_ref, ids_ref, gate_ref,
    wo_hbm, wg_hbm, wu_hbm, wd_hbm,
    out_ref,
    kbuf, vbuf, att, first, outbox, arrived, returned, pack, comb_hi, comb_lo,
    ids_far, gate_far, rows_own, rows_far, part_own, part_far, x_send, x_recv,
    wo, wg, wu, wd, w_sem,
    ks_send, ks_recv, vs_send, vs_recv, d_send, d_recv, r_send, r_recv,
):
    sp = lax.axis_index("sp")
    dp = lax.axis_index("dp")
    tok, q_width = q_ref.shape
    kv_width = k_ref.shape[1]
    head = qg_ref.shape[1]
    d_model = res_ref.shape[1]
    heads_q, heads_kv = q_width // head, kv_width // head
    group = heads_q // heads_kv

    weights = [
        pltpu.make_async_copy(src, dst, w_sem.at[n])
        for n, (src, dst) in enumerate(((wo_hbm, wo), (wg_hbm, wg), (wu_hbm, wu), (wd_hbm, wd)))
    ]
    for w in weights:
        w.start()

    span = n_sp // 2
    n_half = span * n_dp
    start = sp // span * span
    place_sp = sp % span
    partner = (lax.rem(sp + span, n_sp), dp)
    base = start * n_dp

    def peer(i):
        return start + lax.rem(place_sp + i // n_dp, span), lax.rem(dp + i % n_dp, n_dp)

    def source(i):
        return (
            start + lax.rem(place_sp + span - i // n_dp, span),
            lax.rem(dp + n_dp - i % n_dp, n_dp),
        )

    barrier = pltpu.get_barrier_semaphore()

    def greet(i, c):
        pl.semaphore_signal(barrier, inc=1, device_id=peer(i), device_id_type=MESH)
        return c

    def greet_far(i, c):
        pl.semaphore_signal(
            barrier, inc=1, device_id=(lax.rem(start + span + i, n_sp), dp), device_id_type=MESH
        )
        return c

    lax.fori_loop(1, n_half, greet, 0)
    lax.fori_loop(0, span, greet_far, 0)

    lane = lax.broadcasted_iota(jnp.int32, (tok, LANES), 1)
    even = lane % 2 == 0
    low = lane % (2 * head) < head
    same = (
        lax.broadcasted_iota(jnp.int32, (LANES, LANES), 0) // head
        == lax.broadcasted_iota(jnp.int32, (LANES, LANES), 1) // head
    ).astype(bf16)
    per_dev = tok // GRID
    cos_t = jnp.concatenate(
        [cc_ref[...] + cr_ref[pl.ds(sp * per_dev + u, 1), :] for u in range(per_dev)], axis=0
    )
    sin_t = jnp.concatenate(
        [sc_ref[...] + sr_ref[pl.ds(sp * per_dev + u, 1), :] for u in range(per_dev)], axis=0
    )

    def turn(x, gain):
        x = x.astype(f32)
        square = x * x
        hi = square.astype(bf16)
        lo = (square - hi.astype(f32)).astype(bf16)
        mean = (dot(hi, same) + dot(lo, same)) * (1.0 / head)
        x = x * lax.rsqrt(mean + eps_norm) * gain
        swapped = jnp.where(even, pltpu.roll(x, LANES - 1, 1), pltpu.roll(x, 1, 1))
        return x * cos_t + swapped * sin_t

    k_gain = jnp.concatenate([kg_ref[...]] * (LANES // head), axis=1)
    q_gain = jnp.concatenate([qg_ref[...]] * (LANES // head), axis=1)
    for c in range(kv_width // LANES):
        cols = slice(c * LANES, (c + 1) * LANES)
        kbuf[0, :, cols] = turn(k_ref[:, cols], k_gain).astype(bf16)
    vbuf[0] = v_ref[...]

    pl.semaphore_wait(barrier, n_half - 1 + span)

    def exchange(n, src, dst):
        return pltpu.make_async_remote_copy(
            src, dst, x_send.at[n], x_recv.at[n], device_id=partner, device_id_type=MESH
        )

    tables_far = [exchange(0, ids_ref, ids_far), exchange(1, gate_ref, gate_far)]
    rows_copy = exchange(2, rows_own, rows_far)
    part_copy = exchange(3, part_own, part_far)
    for copy in tables_far:
        copy.start()

    def kv_copies(i):
        to = (lax.rem(sp + i, n_sp), dp)
        return (
            pltpu.make_async_remote_copy(
                kbuf.at[0], kbuf.at[i], ks_send.at[i], ks_recv.at[i], device_id=to, device_id_type=MESH
            ),
            pltpu.make_async_remote_copy(
                v_ref, vbuf.at[i], vs_send.at[i], vs_recv.at[i], device_id=to, device_id_type=MESH
            ),
        )

    def kv_start(i, c):
        a, b = kv_copies(i)
        a.start()
        b.start()
        return c

    lax.fori_loop(1, n_sp, kv_start, 0)

    q_rows = [[] for _ in range(heads_kv)]
    per_chunk = LANES // head
    for c in range(q_width // LANES):
        x = turn(q_ref[:, c * LANES : (c + 1) * LANES], q_gain) * head ** (-0.5)
        for part in range(per_chunk):
            kv = (c * per_chunk + part) // group
            want = kv % per_chunk
            y = x if part == want else pltpu.roll(x, head, 1)
            keep = low if want == 0 else jnp.logical_not(low)
            q_rows[kv].append(jnp.where(keep, y, 0.0).astype(bf16))

    n_slot = n_half * pitch
    e_iota = lax.broadcasted_iota(jnp.int32, (n_half, tok), 0) + base
    before = (
        lax.broadcasted_iota(jnp.int32, (tok, tok), 0) < lax.broadcasted_iota(jnp.int32, (tok, tok), 1)
    ).astype(bf16)
    spread = (
        lax.broadcasted_iota(jnp.int32, (n_slot, n_half), 0) // pitch
        == lax.broadcasted_iota(jnp.int32, (n_slot, n_half), 1)
    ).astype(bf16)
    place = (lax.broadcasted_iota(jnp.int32, (n_slot, tok), 0) % pitch + 1).astype(f32)

    def route(n, ids, gates):
        hit0 = (e_iota == ids[0:1, :]).astype(f32)
        hit1 = (e_iota == ids[1:2, :]).astype(f32)
        hits = hit0 + hit1
        rank = dot(hits.astype(bf16), before)
        mark = (hits * (rank + 1.0)).astype(bf16)
        chosen = dot(spread, mark) == place
        pack[n] = chosen.astype(f32).astype(bf16)
        g = gates[...]
        g_hi = g.astype(bf16).astype(f32)
        g_lo = g - g_hi
        for dst, part in ((comb_hi, g_hi), (comb_lo, g_lo)):
            both = (hit0 * part[0:1, :] + hit1 * part[1:2, :]).astype(bf16)
            dst[n] = jnp.where(chosen, dot(spread, both), 0.0).astype(bf16)

    route(0, ids_ref, gate_ref)
    for copy in tables_far:
        copy.wait()
    route(1, ids_far, gate_far)

    def kv_wait(i, c):
        a, b = kv_copies(i)
        a.wait()
        b.wait()
        return c

    lax.fori_loop(1, n_sp, kv_wait, 0)

    keys = n_sp * tok
    outs = {}
    for kv in range(heads_kv):
        cols = slice(kv // per_chunk * LANES, (kv // per_chunk + 1) * LANES)
        k_all = kbuf[:, :, cols].reshape(keys, LANES)
        v_all = vbuf[:, :, cols].reshape(keys, LANES)
        for part in range(group):
            s = lax.dot_general(
                q_rows[kv][part], k_all, (((1,), (1,)), ((), ())), preferred_element_type=f32
            )
            p = jnp.exp(s - jnp.max(s, axis=-1, keepdims=True))
            total = jnp.sum(p, axis=-1, keepdims=True)
            outs[kv * group + part] = dot(p.astype(bf16), v_all) / total
    for c in range(q_width // LANES):
        piece = None
        for part in range(per_chunk):
            h = c * per_chunk + part
            have = (h // group) % per_chunk
            y = outs[h] if part == have else pltpu.roll(outs[h], head, 1)
            piece = y if piece is None else jnp.where(low, piece, y)
        att[:, c * LANES : (c + 1) * LANES] = piece.astype(bf16)

    weights[0].wait()
    projected = dot(att[...], wo[...])
    mixed = (res_ref[...].astype(f32) + rms(projected) * mix_ref[...]).astype(bf16)
    first[...] = mixed
    rows_own[...] = (rms(mixed.astype(f32)) * ffn_ref[...]).astype(bf16)
    rows_copy.start()

    me = place_sp * n_dp + dp

    def dispatch(n, i):
        to = peer(i)
        return pltpu.make_async_remote_copy(
            outbox.at[n, (to[0] - start) * n_dp + to[1]], arrived.at[n, i],
            d_send.at[n, i], d_recv.at[n, i], device_id=to, device_id_type=MESH,
        )

    def answer(n, i):
        return pltpu.make_async_remote_copy(
            arrived.at[n, i], returned.at[n, me], r_send.at[n, i], r_recv.at[n, i],
            device_id=source(i), device_id_type=MESH,
        )

    def each(make, act, n, lo_, hi_):
        def step(i, c):
            copy = make(n, i)
            copy.start() if act == "start" else copy.wait()
            return c

        lax.fori_loop(max(lo_, 1), hi_, step, 0)

    def send_rows(n, rows):
        outbox[n] = dot(pack[n], rows).astype(bf16).reshape(n_half, pitch, d_model)
        mid = n_half // 2
        each(dispatch, "start", n, mid, n_half)
        each(dispatch, "start", n, 0, mid)
        arrived[n, 0] = outbox[n, me]

    def experts(n, lo_, hi_):
        x = arrived[n, lo_:hi_].reshape((hi_ - lo_) * pitch, d_model)
        gate_value = dot(x, wg[...])
        up_value = dot(x, wu[...])
        hidden = (gate_value / (1.0 + jnp.exp(-gate_value)) * up_value).astype(bf16)
        y = dot(hidden, wd[...]).astype(bf16)
        arrived[n, lo_:hi_] = y.reshape(hi_ - lo_, pitch, d_model)

    def combine(n):
        back = returned[n].reshape(n_slot, d_model)
        dims = (((0,), (0,)), ((), ()))
        total = lax.dot_general(comb_hi[n], back, dims, preferred_element_type=f32)
        return total + lax.dot_general(comb_lo[n], back, dims, preferred_element_type=f32)

    send_rows(0, rows_own[...])
    for w in weights[1:]:
        w.wait()
    rows_copy.wait()
    send_rows(1, rows_far[...])
    each(dispatch, "wait", 0, 0, n_half)
    experts(0, 0, n_half)
    mid = n_half // 2
    for lo_, hi_ in ((mid, n_half), (0, mid)):
        each(dispatch, "wait", 1, lo_, hi_)
        experts(1, lo_, hi_)
        each(answer, "start", 1, lo_, hi_)
    each(answer, "start", 0, 0, n_half)
    for n in (0, 1):
        returned[n, me] = arrived[n, 0]
    each(answer, "wait", 1, 0, n_half)
    part_own[...] = combine(1).astype(bf16)
    part_copy.start()
    each(answer, "wait", 0, 0, n_half)
    near = combine(0)
    part_copy.wait()
    expert_sum = near + part_far[...].astype(f32)
    out_ref[...] = (first[...].astype(f32) + rms(expert_sum) * post_ref[...]).astype(bf16)


def shards(
    queries, keys, values, q_gain, k_gain, residual, out_weight, mix_gain, ffn_gain, post_gain,
    expert_ids, expert_gate, w_gate, w_up, w_down,
):
    n_sp = lax.axis_size("sp")
    n_dp = lax.axis_size("dp")
    n_dev = n_sp * n_dp
    tok = queries.shape[1]
    d_model = residual.shape[2]
    d_exp = w_gate.shape[2]
    head = q_gain.shape[0]
    kv_width = keys.shape[2]
    q_width = queries.shape[2]
    cap = 2 * tok * expert_ids.shape[2] // n_dev
    pitch = -(-cap // 16) * 16
    n_half = n_dev // 2
    n_slot = n_half * pitch
    top = expert_ids.shape[2]
    vmem = pl.BlockSpec(memory_space=pltpu.VMEM)
    hbm = pl.BlockSpec(memory_space=pl.ANY)
    dma = pltpu.SemaphoreType.DMA
    result = pl.pallas_call(
        functools.partial(kernel, n_sp, n_dp, pitch),
        out_shape=jax.ShapeDtypeStruct((tok, d_model), bf16),
        in_specs=[vmem] * 15 + [hbm] * 4,
        out_specs=vmem,
        scratch_shapes=[
            pltpu.VMEM((n_sp, tok, kv_width), bf16),
            pltpu.VMEM((n_sp, tok, kv_width), bf16),
            pltpu.VMEM((tok, q_width), bf16),
            pltpu.VMEM((tok, d_model), bf16),
            pltpu.VMEM((2, n_half, pitch, d_model), bf16),
            pltpu.VMEM((2, n_half, pitch, d_model), bf16),
            pltpu.VMEM((2, n_half, pitch, d_model), bf16),
            pltpu.VMEM((2, n_slot, tok), bf16),
            pltpu.VMEM((2, n_slot, tok), bf16),
            pltpu.VMEM((2, n_slot, tok), bf16),
            pltpu.VMEM((top, tok), jnp.int32),
            pltpu.VMEM((top, tok), f32),
            pltpu.VMEM((tok, d_model), bf16),
            pltpu.VMEM((tok, d_model), bf16),
            pltpu.VMEM((tok, d_model), bf16),
            pltpu.VMEM((tok, d_model), bf16),
            dma((4,)), dma((4,)),
            pltpu.VMEM((q_width, d_model), bf16),
            pltpu.VMEM((d_model, d_exp), bf16),
            pltpu.VMEM((d_model, d_exp), bf16),
            pltpu.VMEM((d_exp, d_model), bf16),
            dma((4,)),
            dma((n_sp,)), dma((n_sp,)), dma((n_sp,)), dma((n_sp,)),
            dma((2, n_half)), dma((2, n_half)), dma((2, n_half)), dma((2, n_half)),
        ],
        compiler_params=pltpu.CompilerParams(
            collective_id=0, has_side_effects=True, vmem_limit_bytes=63000000
        ),
    )(
        queries[0], keys[0], values[0], q_gain[None], k_gain[None],
        *tables(n_sp * tok // GRID, head),
        residual[0], mix_gain[None], ffn_gain[None], post_gain[None],
        expert_ids[0].T, expert_gate[0].T,
        out_weight, w_gate[0], w_up[0], w_down[0],
    )
    return result[None]


def solution(mesh):
    tokens = P("dp", "sp", None)
    experts = P(("sp", "dp"), None, None)
    return jax.shard_map(
        shards,
        mesh=mesh,
        in_specs=(tokens, tokens, tokens, P(), P(), tokens, P(), P(), P(), P(), tokens, tokens,
                  experts, experts, experts),
        out_specs=tokens,
        check_vma=False,
    )
```
